512 devices in a mesh: grp: 2 (over y), sp: 32 (over z), tp: 8 (over x, core).
Axes of the slice: x: 4, y: 2, z: 32, core: 2. Of those that a mesh axis runs over, the one named last changes fastest.
The devices are a block of a 4x8x32 slice.
Arguments:
- stream: bfloat16 [49152, 4096], P(('grp', 'sp'), 'tp'), parts along dimension 0, may hold values from -400 to 400
- in_weight: bfloat16 [2, 1024, 4096], P(None, 'sp', 'tp'), may hold values from -0.09375 to 0.09375
- out_weight: bfloat16 [2, 1024, 4096], P(None, 'sp', 'tp'), may hold values from -0.1875 to 0.1875
- group_mix: bfloat16 [2, 4, 256, 256], replicated, may hold values from -0.375 to 0.375
- pool_gain: float32 [2, 1024], replicated, may hold values from 0.1 to 1.9
- norm_gain: float32 [2, 4096], P(None, 'tp'), may hold values from 0.1 to 1.9
- norm_shift: float32 [2, 4096], P(None, 'tp'), may hold values from -3 to 3
Outputs:
- refined: bfloat16 [49152, 4096], P(('grp', 'sp'), 'tp'), parts along dimension 0
The draws below stay inside these ranges and needn't reach their ends.
There are 2 independent parts, one for each index of `grp`. The reference program is written for one: setup_inputs(seed, part) draws one part's arguments, and reference() takes and returns one part's arrays. A program takes and returns all parts, laid end to end along the dimension named above; an argument that names none is the same for every part. Nothing has to cross between parts.
All inputs are finite; a program needn't handle non-finite values.
Results may differ from the reference program's by a relative error of at most 0.015.
Values may be sent and summed in bfloat16 or wider, within the bound.
A program may use at most 64 MiB of HBM per device.

```python
import jax
import jax.numpy as jnp
from jax import lax

D = 4096
POOL = 1024
GROUPS = 4
GROUP_WIDTH = 256
LAYERS = 2
TOKENS = 24576
N_TP = 8


def draw_stream(key, part):
    base = jax.random.fold_in(key, 17)
    first_key, second_key = jax.random.split(base, 2)
    column = jnp.arange(D, dtype=jnp.float32) / D
    row_scale = 10.0 ** jax.random.uniform(second_key, (TOKENS, 1), jnp.float32)
    entries = jnp.clip(jax.random.normal(first_key, (TOKENS, D), jnp.float32), -4.0, 4.0)
    column_scale = 10.0 ** column
    return (entries * column_scale[None, :] * row_scale).astype(jnp.bfloat16)


def steps_of(rng, extent, cuts, smallest, high):
    factor_of, own = 1.0, jax.random.fold_in(rng, 6)
    for axis_at, shards_of in cuts:
        steps = jnp.exp(jax.random.uniform(jax.random.fold_in(own, axis_at), (shards_of,), jnp.float32, smallest / len(cuts), high / len(cuts)))
        factor_of = factor_of * jnp.repeat(steps, extent[axis_at] // shards_of).reshape([-1 if axis == axis_at else 1 for axis in range(len(extent))])
    return factor_of


def centred(stream_key, dims, scale, bound, cuts=(), kind=jnp.bfloat16):
    array = jax.random.normal(stream_key, dims, jnp.float32) * scale
    if len(cuts) > 0:
        array = steps_of(stream_key, dims, cuts, -0.22, 0.18) * array
    return jnp.clip(array, min=-bound, max=bound).astype(kind)


def setup_inputs(seed: int = 0, part: int = 0) -> dict:
    seeds = jax.random.split(jax.random.key(seed), 8)
    own_keys = jax.random.split(jax.random.fold_in(seeds[7], part), 8)
    return {
        "stream": draw_stream(jax.random.fold_in(jax.random.fold_in(seeds[7], part), 71), part),
        "in_weight": centred(seeds[1], (LAYERS, POOL, D), D ** -0.5, 0.09375, ((1, 32), (2, 8))),
        "out_weight": centred(seeds[2], (LAYERS, POOL, D), POOL ** -0.5, 0.1875, ((1, 32), (2, 8))),
        "group_mix": centred(seeds[3], (LAYERS, GROUPS, GROUP_WIDTH, GROUP_WIDTH), GROUP_WIDTH ** -0.5, 0.375),
        "pool_gain": jnp.clip(1.0 + 0.18 * jax.random.normal(seeds[4], (LAYERS, POOL), jnp.float32), 0.1, 1.9),
        "norm_gain": jnp.clip(1.0 + 0.18 * jax.random.normal(seeds[5], (LAYERS, D), jnp.float32), 0.1, 1.9),
        "norm_shift": centred(seeds[6], (LAYERS, D), 0.5, 3.0, ((1, 8),), jnp.float32),
    }


epsilon = 1e-05

def reference(stream, in_weight, out_weight, group_mix, pool_gain, norm_gain, norm_shift):
    tokens_total = stream.shape[0]
    channel_block = D // N_TP
    alpha = (2.0 * LAYERS) ** 0.25
    current = stream
    for layer_index in range(LAYERS):
        hidden_sum = jnp.zeros((tokens_total, POOL), jnp.float32)
        for part_index in range(N_TP):
            lower = part_index * channel_block
            upper = lower + channel_block
            term = jnp.dot(current[:, lower:upper], in_weight[layer_index][:, lower:upper].T, preferred_element_type=jnp.float32)
            rounded = lax.optimization_barrier(term.astype(jnp.bfloat16))
            hidden_sum = hidden_sum + rounded.astype(jnp.float32)
        hidden = hidden_sum.astype(jnp.bfloat16)
        positions = jnp.arange(1, tokens_total + 1, dtype=jnp.float32)[:, None]
        pooled_pieces = []
        for group_index in range(GROUPS):
            width = 2 ** (group_index + 1)
            group_cols = hidden[:, group_index * GROUP_WIDTH:(group_index + 1) * GROUP_WIDTH].astype(jnp.float32)
            padded = jnp.pad(group_cols, ((width - 1, 0), (0, 0)))
            window_sum = jnp.zeros_like(group_cols)
            for offset in range(width):
                window_sum = window_sum + padded[offset:offset + tokens_total]
            counts = jnp.minimum(positions, float(width))
            pooled_pieces.append(window_sum / counts - group_cols)
        pooled = jnp.concatenate(pooled_pieces, axis=1).astype(jnp.bfloat16)
        mixed_pieces = []
        for group_index in range(GROUPS):
            group_rows = pooled[:, group_index * GROUP_WIDTH:(group_index + 1) * GROUP_WIDTH]
            mixed_pieces.append(jnp.dot(group_rows, group_mix[layer_index, group_index], preferred_element_type=jnp.float32))
        scaled = (jnp.concatenate(mixed_pieces, axis=1) * pool_gain[layer_index][None, :]).astype(jnp.bfloat16)
        branch = jnp.dot(scaled, out_weight[layer_index], preferred_element_type=jnp.float32)
        summed = alpha * current.astype(jnp.float32) + branch
        row_mean = lax.optimization_barrier(jnp.sum(summed, axis=1)) / D
        row_var = lax.optimization_barrier(jnp.sum(summed * summed, axis=1)) / D - row_mean * row_mean
        normed = (summed - row_mean[:, None]) * lax.rsqrt(row_var + epsilon)[:, None]
        current = (normed * norm_gain[layer_index][None, :] + norm_shift[layer_index][None, :]).astype(jnp.bfloat16)
    return current
```

```python
import functools

import jax
import jax.numpy as jnp
from jax import lax
from jax.experimental import pallas as pl
from jax.experimental.pallas import tpu as pltpu
from jax.sharding import PartitionSpec as P

D = 4096
GROUPS = 4
GROUP_WIDTH = 256
LAYERS = 2
HALF = GROUP_WIDTH // 2
REACH = 16
HALO = LAYERS * REACH
MESH = pl.DeviceIdType.MESH

epsilon = 1e-05


def kernel(
    n_sp,
    n_tp,
    stream_ref,
    in_ref,
    out_w_ref,
    mix_ref,
    gain_ref,
    norm_gain_ref,
    norm_shift_ref,
    out_ref,
    weights,
    cur,
    band,
    part,
    peer,
    own,
    first,
    second_out,
    second,
    gath,
    summed,
    stat_out,
    stat_in,
    ring_send,
    ring_recv,
    halo_sem,
    part_send,
    part_recv,
    first_send,
    first_recv,
    second_send,
    second_recv,
    gath_send,
    gath_recv,
    stat_send,
    stat_recv,
):
    rows = stream_ref.shape[0]
    block = in_ref.shape[1]
    share = (rows + REACH) // 2 - REACH // 2
    taken = share + HALO
    given = share + REACH
    z = lax.axis_index("sp")
    me = lax.axis_index("tp")
    core = lax.rem(me, 2)
    x = me // 2
    mate = me + 1 - 2 * core
    xa = x + 1 - 2 * lax.rem(x, 2)
    xb = GROUPS - 1 - x
    xo = lax.rem(x + 2, GROUPS)
    dev_a = 2 * xa + core
    dev_b = 2 * xb + core
    right = lax.rem(z + 1, n_sp)
    left = lax.rem(z + n_sp - 1, n_sp)
    alpha = (2.0 * LAYERS) ** 0.25

    barrier = pltpu.get_barrier_semaphore()
    for neighbour in (left, right):
        pl.semaphore_signal(barrier, inc=1, device_id={"sp": neighbour}, device_id_type=MESH)
    for step in range(1, n_tp):
        pl.semaphore_signal(
            barrier, inc=1, device_id={"tp": lax.rem(me + step, n_tp)}, device_id_type=MESH
        )
    pl.semaphore_wait(barrier, 2 + n_tp - 1)

    steps = (n_sp // 2, (n_sp - 1) // 2)

    def at(array, owner):
        return weights.at[array, pl.ds(pl.multiple_of(owner * block, block), block)]

    def owner_of(way, distance):
        if way == 0:
            return lax.rem(z - distance + n_sp, n_sp)
        return lax.rem(z + distance, n_sp)

    def ring_copy(way, array, step, src):
        there = at(array, owner_of(way, step - 1))
        return pltpu.make_async_remote_copy(
            src_ref=there if src is None else src,
            dst_ref=there,
            send_sem=ring_send.at[way, array, step - 1],
            recv_sem=ring_recv.at[way, array, step - 1],
            device_id={"sp": right if way == 0 else left},
            device_id_type=MESH,
        )

    def ring_wait(way, array, step):
        here = at(array, owner_of(way, step))
        pltpu.make_async_remote_copy(
            src_ref=here,
            dst_ref=here,
            send_sem=ring_send.at[way, array, step - 1],
            recv_sem=ring_recv.at[way, array, step - 1],
            device_id={"sp": right if way == 0 else left},
            device_id_type=MESH,
        ).wait_recv()

    halo = pltpu.make_async_remote_copy(
        src_ref=stream_ref.at[pl.ds(rows - HALO, HALO)],
        dst_ref=cur.at[pl.ds(0, HALO)],
        send_sem=halo_sem.at[0],
        recv_sem=halo_sem.at[1],
        device_id={"sp": right},
        device_id_type=MESH,
    )
    sources = [in_ref.at[0], out_w_ref.at[0], in_ref.at[1], out_w_ref.at[1]]
    for array, source in enumerate(sources):
        for way in range(2):
            if steps[way] > 0:
                ring_copy(way, array, 1, source).start()
        if array == 0:
            halo.start()
    for array, source in enumerate(sources):
        at(array, z)[...] = source[...]
    cur[pl.ds(HALO, rows), :] = stream_ref[...]

    window = 2 * jnp.where(x == 0, 1, jnp.where(x == 1, 2, jnp.where(x == 2, 4, 8)))
    start = z * rows - HALO + core * share
    r = lax.broadcasted_iota(jnp.int32, (given, taken), 0) + REACH
    j = lax.broadcasted_iota(jnp.int32, (given, taken), 1)
    count = jnp.clip(start + r + 1, 1, window)
    inside = (r - j >= 0) & (r - j < window) & (start + j >= 0)
    entry = jnp.where(inside, 1.0, 0.0) - jnp.where(r == j, count.astype(jnp.float32), 0.0)
    band[...] = entry.astype(jnp.bfloat16)
    column = lax.broadcasted_iota(jnp.int32, (given, 1), 0) + REACH + start + 1
    scale = 1.0 / jnp.clip(column, 1, window).astype(jnp.float32)

    def forward(step, carry):
        for array in range(2 * LAYERS):
            for way in range(2):
                ring_wait(way, array, step)
                ring_copy(way, array, step + 1, None).start()
        return carry

    if steps[1] > 1:
        lax.fori_loop(1, steps[1], forward, 0)
    for array in range(2 * LAYERS):
        for way in range(2):
            if steps[way] > max(steps[1], 1):
                ring_wait(way, array, steps[way] - 1)
                ring_copy(way, array, steps[way], None).start()
    for array in range(2 * LAYERS):
        for way in range(2):
            if steps[way] > 0:
                ring_wait(way, array, steps[way])
    halo.wait_recv()

    sent = []

    def send(src, dst, sems, to, index):
        copy = pltpu.make_async_remote_copy(
            src_ref=src,
            dst_ref=dst,
            send_sem=sems[0].at[index[0]],
            recv_sem=sems[1].at[index[1]],
            device_id={"tp": to},
            device_id_type=MESH,
        )
        copy.start()
        sent.append(copy)

    def arrive(dst, sems, index):
        pltpu.make_async_remote_copy(
            src_ref=dst,
            dst_ref=dst,
            send_sem=sems[0].at[index[0]],
            recv_sem=sems[1].at[index[1]],
            device_id={"tp": mate},
            device_id_type=MESH,
        ).wait_recv()

    contract_cols = (((1,), (1,)), ((), ()))
    contract = (((1,), (0,)), ((), ()))
    mine = pl.multiple_of(core * share, REACH)
    mates = pl.multiple_of((1 - core) * share, REACH)
    rblock = (rows + REACH) // 7
    eye = lax.broadcasted_iota(jnp.int32, (rblock, 128), 0) == lax.broadcasted_iota(
        jnp.int32, (rblock, 128), 1
    )

    for layer in range(LAYERS):
        order = (xo, xa, xb, x)

        def in_weight_of(g):
            return weights[2 * layer, pl.ds(pl.multiple_of(g * GROUP_WIDTH, GROUP_WIDTH), GROUP_WIDTH)]

        for k, g in enumerate(order):
            product = lax.dot_general(
                cur[pl.ds(mates, taken)], in_weight_of(g), contract_cols,
                preferred_element_type=jnp.float32,
            )
            part[layer, k] = product.astype(jnp.bfloat16)
            send(part.at[layer, k], peer.at[layer, k], (part_send, part_recv), mate,
                 ((layer, k), (layer, k)))
        for k, g in enumerate(order):
            product = lax.dot_general(
                cur[pl.ds(mine, taken)], in_weight_of(g), contract_cols,
                preferred_element_type=jnp.float32,
            )
            arrive(peer.at[layer, k], (part_send, part_recv), ((layer, k), (layer, k)))
            total = (product + peer[layer, k].astype(jnp.float32)).astype(jnp.bfloat16)
            own[layer, k, 0] = total[:, :HALF]
            own[layer, k, 1] = total[:, HALF:]
            f = (first_send, first_recv)
            if k == 0:
                send(own.at[layer, 0, 0], first.at[layer, 0, 1], f, dev_a, ((layer, 0, 1), (layer, 0, 1)))
                send(own.at[layer, 0, 1], first.at[layer, 1, 1], f, dev_b, ((layer, 1, 1), (layer, 1, 1)))
            if k == 1:
                send(own.at[layer, 1, 0], first.at[layer, 0, 0], f, dev_a, ((layer, 0, 0), (layer, 0, 0)))
            if k == 2:
                send(own.at[layer, 2, 1], first.at[layer, 1, 0], f, dev_b, ((layer, 1, 0), (layer, 1, 0)))

        f = (first_send, first_recv)
        s = (second_send, second_recv)
        for half, k, to in ((0, 2, dev_b), (1, 1, dev_a)):
            arrive(first.at[layer, half, 1], f, ((layer, half, 1), (layer, half, 1)))
            second_out[layer, half] = (
                own[layer, k, half].astype(jnp.float32) + first[layer, half, 1].astype(jnp.float32)
            ).astype(jnp.bfloat16)
            send(second_out.at[layer, half], second.at[layer, half], s, to, ((layer, half), (layer, half)))
        pieces = []
        for half in range(2):
            arrive(first.at[layer, half, 0], f, ((layer, half, 0), (layer, half, 0)))
            arrive(second.at[layer, half], s, ((layer, half), (layer, half)))
            pieces.append(
                (
                    own[layer, 3, half].astype(jnp.float32)
                    + first[layer, half, 0].astype(jnp.float32)
                    + second[layer, half].astype(jnp.float32)
                ).astype(jnp.bfloat16)
            )
        hidden = jnp.concatenate(pieces, axis=1)
        pooled = lax.dot_general(band[...], hidden, contract, preferred_element_type=jnp.float32)
        pooled = (pooled * scale).astype(jnp.bfloat16)
        mixed = lax.dot_general(pooled, mix_ref[layer, x], contract, preferred_element_type=jnp.float32)
        scaled = (mixed * gain_ref[layer, x]).astype(jnp.bfloat16)
        gath[layer, core, x, 0] = scaled[:, :HALF]
        gath[layer, core, x, 1] = scaled[:, HALF:]

        def pass_on(g, half, to, slot):
            ref = gath.at[layer, core, g, half]
            send(ref, ref, (gath_send, gath_recv), to, ((layer, slot), (layer, core, g, half)))

        def take_in(side, g, half):
            arrive(gath.at[layer, side, g, half], (gath_send, gath_recv),
                   ((layer, 0), (layer, side, g, half)))

        pass_on(x, 0, dev_b, 0)
        pass_on(x, 1, dev_a, 1)
        pass_on(x, 0, dev_a, 2)
        pass_on(x, 1, dev_b, 3)
        pass_on(x, 0, mate, 4)
        pass_on(x, 1, mate, 5)
        take_in(core, xb, 0)
        pass_on(xb, 0, dev_a, 6)
        take_in(core, xa, 1)
        pass_on(xa, 1, dev_b, 7)
        pass_on(xb, 0, mate, 8)
        pass_on(xa, 1, mate, 9)
        take_in(core, xa, 0)
        pass_on(xa, 0, mate, 10)
        take_in(core, xb, 1)
        pass_on(xb, 1, mate, 11)
        take_in(core, xo, 0)
        pass_on(xo, 0, mate, 12)
        take_in(core, xo, 1)
        pass_on(xo, 1, mate, 13)

        def branch_of(side):
            whole = jnp.concatenate(
                [gath[layer, side, g, half] for g in range(GROUPS) for half in range(2)], axis=1
            )
            return lax.dot_general(
                whole, weights[2 * layer + 1], contract, preferred_element_type=jnp.float32
            )

        summed[pl.ds(mine, given), :] = branch_of(core)
        for g in (x, xb, xa, xo):
            for half in range(2):
                take_in(1 - core, g, half)
        summed[pl.ds(mates, given), :] = branch_of(1 - core)

        stat_out[layer] = jnp.zeros((16, 128), jnp.float32)
        for b in range(7):
            here = pl.ds(b * rblock, rblock)
            value = summed[here, :] + alpha * cur[pl.ds(REACH + b * rblock, rblock), :].astype(jnp.float32)
            summed[here, :] = value
            for at_row, quantity in ((b, value), (8 + b, value * value)):
                total = jnp.sum(quantity, axis=1, keepdims=True)
                stat_out[layer, pl.ds(at_row, 1), :] = jnp.sum(
                    jnp.where(eye, total, 0.0), axis=0, keepdims=True
                )
        q = (stat_send, stat_recv)
        for step in range(1, n_tp):
            to = lax.rem(me + step, n_tp)
            send(stat_out.at[layer], stat_in.at[layer, me], q, to, ((layer, step), (layer, me)))
        stat_in[layer, me] = stat_out[layer]
        for step in range(1, n_tp):
            other = lax.rem(me + step, n_tp)
            arrive(stat_in.at[layer, other], q, ((layer, step), (layer, other)))
        stats = stat_in[layer, 0]
        for k in range(1, n_tp):
            stats = stats + stat_in[layer, k]
        mean = stats[0:8] / D
        var = stats[8:16] / D - mean * mean
        inverse = lax.rsqrt(var + epsilon)
        norm_gain = norm_gain_ref[pl.ds(layer, 1), :]
        norm_shift = norm_shift_ref[pl.ds(layer, 1), :]
        for b in range(7):
            mean_col = jnp.sum(jnp.where(eye, mean[b : b + 1], 0.0), axis=1, keepdims=True)
            inv_col = jnp.sum(jnp.where(eye, inverse[b : b + 1], 0.0), axis=1, keepdims=True)
            value = summed[pl.ds(b * rblock, rblock), :]
            value = (value - mean_col) * inv_col * norm_gain + norm_shift
            if layer < LAYERS - 1:
                cur[pl.ds(REACH + b * rblock, rblock), :] = value.astype(jnp.bfloat16)
            elif b == 0:
                out_ref[pl.ds(0, rblock - REACH), :] = value[REACH:].astype(jnp.bfloat16)
            else:
                out_ref[pl.ds(b * rblock - REACH, rblock), :] = value.astype(jnp.bfloat16)

    for copy in sent:
        copy.wait_send()
    halo.wait_send()

    def drain(step, carry):
        for array in range(2 * LAYERS):
            for way in range(2):
                ring_copy(way, array, step, None).wait_send()
        return carry

    if steps[1] > 0:
        lax.fori_loop(1, steps[1] + 1, drain, 0)
    for array in range(2 * LAYERS):
        if steps[0] > steps[1]:
            ring_copy(0, array, steps[0], None).wait_send()


def per_device(n_sp, n_tp, stream, in_weight, out_weight, group_mix, pool_gain, norm_gain, norm_shift):
    rows, cols = stream.shape
    pool = GROUPS * GROUP_WIDTH
    share = (rows + REACH) // 2 - REACH // 2
    taken, given = share + HALO, share + REACH
    bf, f32 = jnp.bfloat16, jnp.float32
    gains = pool_gain.reshape(LAYERS, GROUPS, 1, GROUP_WIDTH)
    steps = max(n_sp // 2, 1)
    dma = pltpu.SemaphoreType.DMA
    return pl.pallas_call(
        functools.partial(kernel, n_sp, n_tp),
        out_shape=jax.ShapeDtypeStruct((rows, cols), bf),
        in_specs=[pl.BlockSpec(memory_space=pltpu.VMEM)] * 7,
        out_specs=pl.BlockSpec(memory_space=pltpu.VMEM),
        scratch_shapes=[
            pltpu.VMEM((2 * LAYERS, pool, cols), bf),
            pltpu.VMEM((rows + HALO, cols), bf),
            pltpu.VMEM((given, taken), bf),
            pltpu.VMEM((LAYERS, GROUPS, taken, GROUP_WIDTH), bf),
            pltpu.VMEM((LAYERS, GROUPS, taken, GROUP_WIDTH), bf),
            pltpu.VMEM((LAYERS, GROUPS, 2, taken, HALF), bf),
            pltpu.VMEM((LAYERS, 2, 2, taken, HALF), bf),
            pltpu.VMEM((LAYERS, 2, taken, HALF), bf),
            pltpu.VMEM((LAYERS, 2, taken, HALF), bf),
            pltpu.VMEM((LAYERS, 2, GROUPS, 2, given, HALF), bf),
            pltpu.VMEM((rows + REACH, cols), f32),
            pltpu.VMEM((LAYERS, 16, 128), f32),
            pltpu.VMEM((LAYERS, n_tp, 16, 128), f32),
            dma((2, 2 * LAYERS, steps)),
            dma((2, 2 * LAYERS, steps)),
            dma((2,)),
            dma((LAYERS, GROUPS)),
            dma((LAYERS, GROUPS)),
            dma((LAYERS, 2, 2)),
            dma((LAYERS, 2, 2)),
            dma((LAYERS, 2)),
            dma((LAYERS, 2)),
            dma((LAYERS, 14)),
            dma((LAYERS, 2, GROUPS, 2)),
            dma((LAYERS, n_tp)),
            dma((LAYERS, n_tp)),
        ],
        compiler_params=pltpu.CompilerParams(
            collective_id=0, has_side_effects=True, vmem_limit_bytes=48 * 1024 * 1024
        ),
    )(stream, in_weight, out_weight, group_mix, gains, norm_gain, norm_shift)


def solution(mesh):
    in_specs = (
        P(("grp", "sp"), "tp"),
        P(None, "sp", "tp"),
        P(None, "sp", "tp"),
        P(),
        P(),
        P(None, "tp"),
        P(None, "tp"),
    )
    out_specs = P(("grp", "sp"), "tp")
    return jax.shard_map(
        functools.partial(per_device, mesh.shape["sp"], mesh.shape["tp"]),
        mesh=mesh, in_specs=in_specs, out_specs=out_specs, check_vma=False,
    )
```

```python
import functools

import jax
import jax.numpy as jnp
from jax import lax
from jax.experimental import pallas as pl
from jax.experimental.pallas import tpu as pltpu
from jax.sharding import PartitionSpec as P

D = 4096
GROUPS = 4
GROUP_WIDTH = 256
LAYERS = 2
HALF = GROUP_WIDTH // 2
REACH = 16
STRIDE = 4
HALO = LAYERS * REACH
MESH = pl.DeviceIdType.MESH

epsilon = 1e-05


def kernel(
    n_sp,
    n_tp,
    stream_hbm,
    in_hbm,
    out_hbm,
    mix_hbm,
    gain_hbm,
    norm_gain_hbm,
    norm_shift_hbm,
    out_ref,
    mix_ref,
    gain_ref,
    norm_gain_ref,
    norm_shift_ref,
    weights,
    cur,
    band,
    part,
    peer,
    own,
    first,
    second_out,
    second,
    gath,
    summed,
    stat_out,
    stat_in,
    load_sem,
    ring_send,
    ring_recv,
    halo_sem,
    part_send,
    part_recv,
    first_send,
    first_recv,
    second_send,
    second_recv,
    gath_send,
    gath_recv,
    stat_send,
    stat_recv,
):
    rows = stream_hbm.shape[0]
    block = in_hbm.shape[1]
    share = (rows + REACH) // 2 - REACH // 2
    taken = share + HALO
    given = share + REACH
    z = lax.axis_index("sp")
    me = lax.axis_index("tp")
    core = lax.rem(me, 2)
    x = me // 2
    mate = me + 1 - 2 * core
    xa = x + 1 - 2 * lax.rem(x, 2)
    xb = GROUPS - 1 - x
    xo = lax.rem(x + 2, GROUPS)
    dev_a = 2 * xa + core
    dev_b = 2 * xb + core
    alpha = (2.0 * LAYERS) ** 0.25

    def load(src, dst, index):
        copy = pltpu.make_async_copy(src, dst, load_sem.at[index])
        copy.start()
        return copy

    own_rows = pl.ds(pl.multiple_of(z * block, block), block)
    loads = [
        load(in_hbm.at[0], weights.at[0, own_rows], 0),
        load(out_hbm.at[0], weights.at[1, own_rows], 1),
        load(in_hbm.at[1], weights.at[2, own_rows], 2),
        load(out_hbm.at[1], weights.at[3, own_rows], 3),
        load(stream_hbm, cur.at[pl.ds(HALO, rows)], 4),
        load(mix_hbm, mix_ref, 5),
        load(gain_hbm, gain_ref, 6),
        load(norm_gain_hbm, norm_gain_ref, 7),
        load(norm_shift_hbm, norm_shift_ref, 8),
    ]

    barrier = pltpu.get_barrier_semaphore()
    for distance in (1, -1, STRIDE, -STRIDE):
        pl.semaphore_signal(
            barrier, inc=1, device_id={"sp": lax.rem(z + distance % n_sp, n_sp)}, device_id_type=MESH
        )
    for step in range(1, n_tp):
        pl.semaphore_signal(
            barrier, inc=1, device_id={"tp": lax.rem(me + step, n_tp)}, device_id_type=MESH
        )
    pl.semaphore_wait(barrier, 4 + n_tp - 1)

    classes = n_sp // STRIDE
    main_steps, back_steps = classes // 2, (classes - 1) // 2

    def at(array, owner):
        return weights.at[array, pl.ds(pl.multiple_of(owner * block, block), block)]

    def along(array, distance):
        sign = 1 if array % 2 == 0 else -1
        return lax.rem(z + (sign * distance) % n_sp, n_sp)

    def hop(array, kind, index, owner, to):
        ref = at(array, owner)
        return pltpu.make_async_remote_copy(
            src_ref=ref,
            dst_ref=ref,
            send_sem=ring_send.at[array, kind, index],
            recv_sem=ring_recv.at[array, kind, index],
            device_id={"sp": to},
            device_id_type=MESH,
        )

    sent_hops = []

    def go(array, kind, index, owner, distance):
        copy = hop(array, kind, index, owner, along(array, distance))
        copy.start()
        sent_hops.append(copy)

    def come(array, kind, index, owner):
        hop(array, kind, index, owner, along(array, 1)).wait_recv()

    def both(k):
        found = [(k, -STRIDE * k)] if k <= main_steps else []
        if 0 < k <= back_steps:
            found.append((classes - k, STRIDE * k))
        return found

    def stride_stage(array, k):
        for index, distance in both(k):
            kind = 0 if distance <= 0 else 1
            owner = along(array, distance)
            if k > 0:
                come(array, kind, k - 1, owner)
            if (kind == 0) and k < main_steps:
                go(array, 0, k, owner, STRIDE)
            if (kind == 1 or k == 0) and k < back_steps:
                go(array, 1, k, owner, -STRIDE)
            go(array, 2, index, owner, 1)
            go(array, 4, index, owner, -1)

    def near_stage(array, k):
        for index, distance in both(k):
            owner = along(array, distance - 1)
            come(array, 2, index, owner)
            go(array, 3, index, owner, 1)

    def last_stage(array):
        for k in range(main_steps + 1):
            for index, distance in both(k):
                come(array, 3, index, along(array, distance - 2))
                come(array, 4, index, along(array, distance + 1))

    def stages(arrays):
        found = []
        for k in range(1, main_steps + 1):
            found.append([functools.partial(stride_stage, array, k) for array in arrays])
            found.append([functools.partial(near_stage, array, k - 1) for array in arrays])
        found.append([functools.partial(near_stage, array, main_steps) for array in arrays])
        return found

    for array in range(2):
        loads[array].wait()
        stride_stage(array, 0)
    loads[4].wait()
    halo = pltpu.make_async_remote_copy(
        src_ref=cur.at[pl.ds(rows, HALO)],
        dst_ref=cur.at[pl.ds(0, HALO)],
        send_sem=halo_sem.at[0],
        recv_sem=halo_sem.at[1],
        device_id={"sp": lax.rem(z + 1, n_sp)},
        device_id_type=MESH,
    )
    halo.start()
    for array in range(2, 4):
        loads[array].wait()
        stride_stage(array, 0)

    window = 2 * jnp.where(x == 0, 1, jnp.where(x == 1, 2, jnp.where(x == 2, 4, 8)))
    start = z * rows - HALO + core * share
    r = lax.broadcasted_iota(jnp.int32, (given, taken), 0) + REACH
    j = lax.broadcasted_iota(jnp.int32, (given, taken), 1)
    count = jnp.clip(start + r + 1, 1, window)
    inside = (r - j >= 0) & (r - j < window) & (start + j >= 0)
    entry = jnp.where(inside, 1.0, 0.0) - jnp.where(r == j, count.astype(jnp.float32), 0.0)
    band[...] = entry.astype(jnp.bfloat16)
    column = lax.broadcasted_iota(jnp.int32, (given, 1), 0) + REACH + start + 1
    scale = 1.0 / jnp.clip(column, 1, window).astype(jnp.float32)

    for stage in stages((0, 1)):
        for part_of in stage:
            part_of()
    later = stages((2, 3))

    def meanwhile(number):
        for _ in range(number):
            if later:
                for part_of in later.pop(0):
                    part_of()

    for load in loads[5:]:
        load.wait()
    last_stage(0)
    halo.wait_recv()

    sent = []

    def send(src, dst, sems, to, index):
        copy = pltpu.make_async_remote_copy(
            src_ref=src,
            dst_ref=dst,
            send_sem=sems[0].at[index[0]],
            recv_sem=sems[1].at[index[1]],
            device_id={"tp": to},
            device_id_type=MESH,
        )
        copy.start()
        sent.append(copy)

    def arrive(dst, sems, index):
        pltpu.make_async_remote_copy(
            src_ref=dst,
            dst_ref=dst,
            send_sem=sems[0].at[index[0]],
            recv_sem=sems[1].at[index[1]],
            device_id={"tp": mate},
            device_id_type=MESH,
        ).wait_recv()

    contract_cols = (((1,), (1,)), ((), ()))
    contract = (((1,), (0,)), ((), ()))
    mine = pl.multiple_of(core * share, REACH)
    mates = pl.multiple_of((1 - core) * share, REACH)
    rblock = (rows + REACH) // 7
    eye = lax.broadcasted_iota(jnp.int32, (rblock, 128), 0) == lax.broadcasted_iota(
        jnp.int32, (rblock, 128), 1
    )

    for layer in range(LAYERS):
        if layer > 0:
            last_stage(2 * layer)
        order = (xo, xa, xb, x)

        def in_weight_of(g):
            return weights[2 * layer, pl.ds(pl.multiple_of(g * GROUP_WIDTH, GROUP_WIDTH), GROUP_WIDTH)]

        for k, g in enumerate(order):
            product = lax.dot_general(
                cur[pl.ds(mates, taken)], in_weight_of(g), contract_cols,
                preferred_element_type=jnp.float32,
            )
            part[layer, k] = product.astype(jnp.bfloat16)
            send(part.at[layer, k], peer.at[layer, k], (part_send, part_recv), mate,
                 ((layer, k), (layer, k)))
        for k, g in enumerate(order):
            product = lax.dot_general(
                cur[pl.ds(mine, taken)], in_weight_of(g), contract_cols,
                preferred_element_type=jnp.float32,
            )
            arrive(peer.at[layer, k], (part_send, part_recv), ((layer, k), (layer, k)))
            total = (product + peer[layer, k].astype(jnp.float32)).astype(jnp.bfloat16)
            own[layer, k, 0] = total[:, :HALF]
            own[layer, k, 1] = total[:, HALF:]
            f = (first_send, first_recv)
            if k == 0:
                send(own.at[layer, 0, 0], first.at[layer, 0, 1], f, dev_a, ((layer, 0, 1), (layer, 0, 1)))
                send(own.at[layer, 0, 1], first.at[layer, 1, 1], f, dev_b, ((layer, 1, 1), (layer, 1, 1)))
            if k == 1:
                send(own.at[layer, 1, 0], first.at[layer, 0, 0], f, dev_a, ((layer, 0, 0), (layer, 0, 0)))
            if k == 2:
                send(own.at[layer, 2, 1], first.at[layer, 1, 0], f, dev_b, ((layer, 1, 0), (layer, 1, 0)))

        f = (first_send, first_recv)
        s = (second_send, second_recv)
        meanwhile(2)
        for half, k, to in ((0, 2, dev_b), (1, 1, dev_a)):
            arrive(first.at[layer, half, 1], f, ((layer, half, 1), (layer, half, 1)))
            second_out[layer, half] = (
                own[layer, k, half].astype(jnp.float32) + first[layer, half, 1].astype(jnp.float32)
            ).astype(jnp.bfloat16)
            send(second_out.at[layer, half], second.at[layer, half], s, to, ((layer, half), (layer, half)))
        meanwhile(2)
        pieces = []
        for half in range(2):
            arrive(first.at[layer, half, 0], f, ((layer, half, 0), (layer, half, 0)))
            arrive(second.at[layer, half], s, ((layer, half), (layer, half)))
            pieces.append(
                (
                    own[layer, 3, half].astype(jnp.float32)
                    + first[layer, half, 0].astype(jnp.float32)
                    + second[layer, half].astype(jnp.float32)
                ).astype(jnp.bfloat16)
            )
        hidden = jnp.concatenate(pieces, axis=1)
        pooled = lax.dot_general(band[...], hidden, contract, preferred_element_type=jnp.float32)
        pooled = (pooled * scale).astype(jnp.bfloat16)
        mixed = lax.dot_general(pooled, mix_ref[layer, x], contract, preferred_element_type=jnp.float32)
        gains = jnp.zeros((1, GROUP_WIDTH), jnp.float32)
        for g in range(GROUPS):
            of_g = gain_ref[pl.ds(layer, 1), pl.ds(g * GROUP_WIDTH, GROUP_WIDTH)]
            gains = jnp.where(x == g, of_g, gains)
        scaled = (mixed * gains).astype(jnp.bfloat16)
        gath[layer, core, x, 0] = scaled[:, :HALF]
        gath[layer, core, x, 1] = scaled[:, HALF:]

        def pass_on(g, half, to, slot):
            ref = gath.at[layer, core, g, half]
            send(ref, ref, (gath_send, gath_recv), to, ((layer, slot), (layer, core, g, half)))

        def take_in(side, g, half):
            arrive(gath.at[layer, side, g, half], (gath_send, gath_recv),
                   ((layer, 0), (layer, side, g, half)))

        pass_on(x, 0, dev_b, 0)
        pass_on(x, 1, dev_a, 1)
        pass_on(x, 0, dev_a, 2)
        pass_on(x, 1, dev_b, 3)
        pass_on(x, 0, mate, 4)
        pass_on(x, 1, mate, 5)
        meanwhile(2)
        take_in(core, xb, 0)
        pass_on(xb, 0, dev_a, 6)
        take_in(core, xa, 1)
        pass_on(xa, 1, dev_b, 7)
        pass_on(xb, 0, mate, 8)
        pass_on(xa, 1, mate, 9)
        meanwhile(2)
        take_in(core, xa, 0)
        pass_on(xa, 0, mate, 10)
        take_in(core, xb, 1)
        pass_on(xb, 1, mate, 11)
        take_in(core, xo, 0)
        pass_on(xo, 0, mate, 12)
        take_in(core, xo, 1)
        pass_on(xo, 1, mate, 13)

        def branch_of(side):
            whole = jnp.concatenate(
                [gath[layer, side, g, half] for g in range(GROUPS) for half in range(2)], axis=1
            )
            return lax.dot_general(
                whole, weights[2 * layer + 1], contract, preferred_element_type=jnp.float32
            )

        last_stage(2 * layer + 1)
        summed[pl.ds(mine, given), :] = branch_of(core)
        for g in (x, xb, xa, xo):
            for half in range(2):
                take_in(1 - core, g, half)
        summed[pl.ds(mates, given), :] = branch_of(1 - core)

        stat_out[layer] = jnp.zeros((16, 128), jnp.float32)
        for b in range(7):
            here = pl.ds(b * rblock, rblock)
            value = summed[here, :] + alpha * cur[pl.ds(REACH + b * rblock, rblock), :].astype(jnp.float32)
            summed[here, :] = value
            for at_row, quantity in ((b, value), (8 + b, value * value)):
                total = jnp.sum(quantity, axis=1, keepdims=True)
                stat_out[layer, pl.ds(at_row, 1), :] = jnp.sum(
                    jnp.where(eye, total, 0.0), axis=0, keepdims=True
                )
        q = (stat_send, stat_recv)
        for step in range(1, n_tp):
            to = lax.rem(me + step, n_tp)
            send(stat_out.at[layer], stat_in.at[layer, me], q, to, ((layer, step), (layer, me)))
        stat_in[layer, me] = stat_out[layer]
        meanwhile(len(later))
        for step in range(1, n_tp):
            other = lax.rem(me + step, n_tp)
            arrive(stat_in.at[layer, other], q, ((layer, step), (layer, other)))
        stats = stat_in[layer, 0]
        for k in range(1, n_tp):
            stats = stats + stat_in[layer, k]
        if layer == 0:
            halo.wait_send()
        mean = stats[0:8] / D
        var = stats[8:16] / D - mean * mean
        inverse = lax.rsqrt(var + epsilon)
        norm_gain = norm_gain_ref[pl.ds(layer, 1), :]
        norm_shift = norm_shift_ref[pl.ds(layer, 1), :]
        for b in range(7):
            mean_col = jnp.sum(jnp.where(eye, mean[b : b + 1], 0.0), axis=1, keepdims=True)
            inv_col = jnp.sum(jnp.where(eye, inverse[b : b + 1], 0.0), axis=1, keepdims=True)
            value = summed[pl.ds(b * rblock, rblock), :]
            value = (value - mean_col) * inv_col * norm_gain + norm_shift
            if layer < LAYERS - 1:
                cur[pl.ds(REACH + b * rblock, rblock), :] = value.astype(jnp.bfloat16)
            elif b == 0:
                out_ref[pl.ds(0, rblock - REACH), :] = value[REACH:].astype(jnp.bfloat16)
            else:
                out_ref[pl.ds(b * rblock - REACH, rblock), :] = value.astype(jnp.bfloat16)

    for copy in sent + sent_hops:
        copy.wait_send()


def per_device(n_sp, n_tp, stream, in_weight, out_weight, group_mix, pool_gain, norm_gain, norm_shift):
    rows, cols = stream.shape
    pool = GROUPS * GROUP_WIDTH
    share = (rows + REACH) // 2 - REACH // 2
    taken, given = share + HALO, share + REACH
    bf, f32 = jnp.bfloat16, jnp.float32
    classes = n_sp // STRIDE
    dma = pltpu.SemaphoreType.DMA
    return pl.pallas_call(
        functools.partial(kernel, n_sp, n_tp),
        out_shape=jax.ShapeDtypeStruct((rows, cols), bf),
        in_specs=[pl.BlockSpec(memory_space=pl.ANY)] * 7,
        out_specs=pl.BlockSpec(memory_space=pltpu.VMEM),
        scratch_shapes=[
            pltpu.VMEM(group_mix.shape, bf),
            pltpu.VMEM(pool_gain.shape, f32),
            pltpu.VMEM(norm_gain.shape, f32),
            pltpu.VMEM(norm_shift.shape, f32),
            pltpu.VMEM((2 * LAYERS, pool, cols), bf),
            pltpu.VMEM((rows + HALO, cols), bf),
            pltpu.VMEM((given, taken), bf),
            pltpu.VMEM((LAYERS, GROUPS, taken, GROUP_WIDTH), bf),
            pltpu.VMEM((LAYERS, GROUPS, taken, GROUP_WIDTH), bf),
            pltpu.VMEM((LAYERS, GROUPS, 2, taken, HALF), bf),
            pltpu.VMEM((LAYERS, 2, 2, taken, HALF), bf),
            pltpu.VMEM((LAYERS, 2, taken, HALF), bf),
            pltpu.VMEM((LAYERS, 2, taken, HALF), bf),
            pltpu.VMEM((LAYERS, 2, GROUPS, 2, given, HALF), bf),
            pltpu.VMEM((rows + REACH, cols), f32),
            pltpu.VMEM((LAYERS, 16, 128), f32),
            pltpu.VMEM((LAYERS, n_tp, 16, 128), f32),
            dma((9,)),
            dma((2 * LAYERS, 5, classes)),
            dma((2 * LAYERS, 5, classes)),
            dma((2,)),
            dma((LAYERS, GROUPS)),
            dma((LAYERS, GROUPS)),
            dma((LAYERS, 2, 2)),
            dma((LAYERS, 2, 2)),
            dma((LAYERS, 2)),
            dma((LAYERS, 2)),
            dma((LAYERS, 14)),
            dma((LAYERS, 2, GROUPS, 2)),
            dma((LAYERS, n_tp)),
            dma((LAYERS, n_tp)),
        ],
        compiler_params=pltpu.CompilerParams(
            collective_id=0, has_side_effects=True, vmem_limit_bytes=60 * 1024 * 1024
        ),
    )(stream, in_weight, out_weight, group_mix, pool_gain, norm_gain, norm_shift)


def solution(mesh):
    in_specs = (
        P(("grp", "sp"), "tp"),
        P(None, "sp", "tp"),
        P(None, "sp", "tp"),
        P(),
        P(),
        P(None, "tp"),
        P(None, "tp"),
    )
    out_specs = P(("grp", "sp"), "tp")
    return jax.shard_map(
        functools.partial(per_device, mesh.shape["sp"], mesh.shape["tp"]),
        mesh=mesh, in_specs=in_specs, out_specs=out_specs, check_vma=False,
    )
```

```python
import functools

import jax
import jax.numpy as jnp
from jax import lax
from jax.experimental import pallas as pl
from jax.experimental.pallas import tpu as pltpu
from jax.sharding import PartitionSpec as P

D = 4096
GROUPS = 4
GROUP_WIDTH = 256
LAYERS = 2
HALF = GROUP_WIDTH // 2
REACH = 16
STRIDE = 4
LAGS = (0, 0, 10, 10)
POLLS = (0, 4, 4, 4, 6, 40)
HALO = LAYERS * REACH
MESH = pl.DeviceIdType.MESH

epsilon = 1e-05


def kernel(
    n_sp,
    n_tp,
    stream_hbm,
    in_hbm,
    out_hbm,
    mix_hbm,
    gain_hbm,
    norm_gain_hbm,
    norm_shift_hbm,
    out_ref,
    mix_ref,
    gain_ref,
    norm_gain_ref,
    norm_shift_ref,
    weights,
    cur,
    band,
    part,
    peer,
    own,
    first,
    second_out,
    second,
    gath,
    summed,
    stat_out,
    stat_in,
    load_sem,
    ring_send,
    ring_recv,
    pair_send,
    pair_recv,
    halo_sem,
    part_send,
    part_recv,
    first_send,
    first_recv,
    second_send,
    second_recv,
    gath_send,
    gath_recv,
    stat_send,
    stat_recv,
):
    rows = stream_hbm.shape[0]
    block = in_hbm.shape[1]
    share = (rows + REACH) // 2 - REACH // 2
    taken = share + HALO
    given = share + REACH
    z = lax.axis_index("sp")
    me = lax.axis_index("tp")
    part_at = lax.axis_index("grp")
    core = lax.rem(me, 2)
    x = me // 2
    mate = me + 1 - 2 * core
    xa = x + 1 - 2 * lax.rem(x, 2)
    xb = GROUPS - 1 - x
    xo = lax.rem(x + 2, GROUPS)
    dev_a = 2 * xa + core
    dev_b = 2 * xb + core
    alpha = (2.0 * LAYERS) ** 0.25

    def load(src, dst, index):
        copy = pltpu.make_async_copy(src, dst, load_sem.at[index])
        copy.start()
        return copy

    own_rows = pl.ds(pl.multiple_of(z * block, block), block)
    loads = [
        load(in_hbm.at[0], weights.at[0, own_rows], 0),
        load(out_hbm.at[0], weights.at[1, own_rows], 1),
        load(in_hbm.at[1], weights.at[2, own_rows], 2),
        load(out_hbm.at[1], weights.at[3, own_rows], 3),
        load(stream_hbm, cur.at[pl.ds(HALO, rows)], 4),
        load(mix_hbm, mix_ref, 5),
        load(gain_hbm, gain_ref, 6),
        load(norm_gain_hbm, norm_gain_ref, 7),
        load(norm_shift_hbm, norm_shift_ref, 8),
    ]

    barrier = pltpu.get_barrier_semaphore()
    reached = (1, -1, STRIDE, -STRIDE)
    for distance in reached:
        pl.semaphore_signal(
            barrier, inc=1, device_id={"sp": lax.rem(z + distance % n_sp, n_sp)}, device_id_type=MESH
        )
    for step in range(1, n_tp):
        pl.semaphore_signal(
            barrier, inc=1, device_id={"tp": lax.rem(me + step, n_tp)}, device_id_type=MESH
        )
    beside = part_at + 1 - 2 * lax.rem(part_at, 2)
    pl.semaphore_signal(barrier, inc=1, device_id={"grp": beside}, device_id_type=MESH)
    pl.semaphore_wait(barrier, len(reached) + 1 + n_tp - 1)

    classes = n_sp // STRIDE
    main_steps, back_steps = classes // 2, (classes - 1) // 2

    def at(array, owner):
        return weights.at[array, pl.ds(pl.multiple_of(owner * block, block), block)]

    def along(distance):
        return lax.rem(z + distance % n_sp, n_sp)

    half_block = block // 2
    carried = lax.rem(part_at, 2)
    beside = part_at + 1 - 2 * carried

    def half_at(array, owner, which):
        start = owner * block + which * half_block
        return weights.at[array, pl.ds(pl.multiple_of(start, half_block), half_block)]

    def across(array, kind, index, owner, which):
        ref = half_at(array, owner, which)
        return pltpu.make_async_remote_copy(
            src_ref=ref,
            dst_ref=ref,
            send_sem=pair_send.at[array, kind, index],
            recv_sem=pair_recv.at[array, kind, index],
            device_id={"grp": beside},
            device_id_type=MESH,
        )

    def hop(array, kind, index, owner, to):
        ref = half_at(array, owner, carried)
        return pltpu.make_async_remote_copy(
            src_ref=ref,
            dst_ref=ref,
            send_sem=ring_send.at[array, kind, index],
            recv_sem=ring_recv.at[array, kind, index],
            device_id={"sp": to},
            device_id_type=MESH,
        )

    sent_hops = []

    def go(array, kind, index, owner, distance):
        copy = hop(array, kind, index, owner, along(distance))
        copy.start()
        sent_hops.append(copy)

    pair_kind = (0, 0, 1, 2, 3)

    def come(array, kind, index, owner):
        hop(array, kind, index, owner, along(1)).wait_recv()

    held_back = [[] for _ in range(2 * LAYERS)]

    def share_out(array, kind, index, owner):
        copy = across(array, pair_kind[kind], index, owner, carried)
        if array == 0:
            copy.start()
        else:
            held_back[array].append(copy)
        sent_hops.append(copy)

    def let_go(arrays):
        for array in arrays:
            for copy in held_back[array]:
                copy.start()
            held_back[array].clear()

    def both(k):
        found = [(k, -STRIDE * k)] if k <= main_steps else []
        if 0 < k <= back_steps:
            found.append((classes - k, STRIDE * k))
        return found

    def stride_stage(array, k):
        for index, distance in both(k):
            kind = 0 if distance <= 0 else 1
            owner = along(distance)
            if k > 0:
                come(array, kind, k - 1, owner)
            if (kind == 0) and k < main_steps:
                go(array, 0, k, owner, STRIDE)
            if (kind == 1 or k == 0) and k < back_steps:
                go(array, 1, k, owner, -STRIDE)
            go(array, 2, index, owner, -1)
            go(array, 4, index, owner, 1)
            if k > 0:
                share_out(array, kind, index, owner)

    def near_stage(array, k):
        for index, distance in both(k):
            owner = along(distance + 1)
            come(array, 2, index, owner)
            go(array, 3, index, owner, -1)
            share_out(array, 2, index, owner)

    def last_stage(array, kind, shift):
        for k in range(main_steps + 1):
            for index, distance in both(k):
                come(array, kind, index, along(distance + shift))
                share_out(array, kind, index, along(distance + shift))

    def pair_stage(array):
        for k in range(main_steps + 1):
            for index, distance in both(k):
                for kind, shift in ((0, 0), (1, 1), (2, 2), (3, -1)):
                    if kind > 0 or k > 0:
                        across(array, kind, index, along(distance + shift), 1 - carried).wait_recv()

    def stages(array):
        found = []
        for k in range(1, main_steps + 1):
            found.append(functools.partial(stride_stage, array, k))
            if k > 1:
                found.append(functools.partial(near_stage, array, k - 2))
        for k in range(max(main_steps - 1, 0), main_steps + 1):
            found.append(functools.partial(near_stage, array, k))
        found.append(functools.partial(last_stage, array, 4, -1))
        found.append(functools.partial(last_stage, array, 3, 2))
        return found

    for array in range(2):
        loads[array].wait()
        stride_stage(array, 0)
    loads[4].wait()
    halo = pltpu.make_async_remote_copy(
        src_ref=cur.at[pl.ds(rows, HALO)],
        dst_ref=cur.at[pl.ds(0, HALO)],
        send_sem=halo_sem.at[0],
        recv_sem=halo_sem.at[1],
        device_id={"sp": lax.rem(z + 1, n_sp)},
        device_id_type=MESH,
    )
    halo.start()
    for array in range(2, 4):
        loads[array].wait()

    window = 2 * jnp.where(x == 0, 1, jnp.where(x == 1, 2, jnp.where(x == 2, 4, 8)))
    start = z * rows - HALO + core * share
    r = lax.broadcasted_iota(jnp.int32, (given, taken), 0) + REACH
    j = lax.broadcasted_iota(jnp.int32, (given, taken), 1)
    count = jnp.clip(start + r + 1, 1, window)
    inside = (r - j >= 0) & (r - j < window) & (start + j >= 0)
    entry = jnp.where(inside, 1.0, 0.0) - jnp.where(r == j, count.astype(jnp.float32), 0.0)
    band[...] = entry.astype(jnp.bfloat16)
    column = lax.broadcasted_iota(jnp.int32, (given, 1), 0) + REACH + start + 1
    scale = 1.0 / jnp.clip(column, 1, window).astype(jnp.float32)

    waves = [stages(array) for array in range(2 * LAYERS)]
    turns = sorted(
        (k + LAGS[array], array, k) for array in range(2 * LAYERS) for k in range(len(waves[array]))
    )
    done = len(waves[0])
    for turn, array, k in turns:
        if turn == 4 and array == 0:
            stride_stage(2, 0)
            stride_stage(3, 0)
        if turn < done:
            waves[array][k]()
    later = [waves[array][k] for turn, array, k in turns if turn >= done]
    polls = list(POLLS)

    def meanwhile(arrays):
        for _ in range(polls.pop(0) if polls else len(later)):
            if later:
                later.pop(0)()
        let_go(arrays)

    for load in loads[5:]:
        load.wait()
    pair_stage(0)
    halo.wait_recv()
    meanwhile((1,))

    sent = []

    def send(src, dst, sems, to, index):
        copy = pltpu.make_async_remote_copy(
            src_ref=src,
            dst_ref=dst,
            send_sem=sems[0].at[index[0]],
            recv_sem=sems[1].at[index[1]],
            device_id={"tp": to},
            device_id_type=MESH,
        )
        copy.start()
        sent.append(copy)

    def arrive(dst, sems, index):
        pltpu.make_async_remote_copy(
            src_ref=dst,
            dst_ref=dst,
            send_sem=sems[0].at[index[0]],
            recv_sem=sems[1].at[index[1]],
            device_id={"tp": mate},
            device_id_type=MESH,
        ).wait_recv()

    contract_cols = (((1,), (1,)), ((), ()))
    contract = (((1,), (0,)), ((), ()))
    mine = pl.multiple_of(core * share, REACH)
    mates = pl.multiple_of((1 - core) * share, REACH)
    rblock = (rows + REACH) // 7
    eye = lax.broadcasted_iota(jnp.int32, (rblock, 128), 0) == lax.broadcasted_iota(
        jnp.int32, (rblock, 128), 1
    )

    for layer in range(LAYERS):
        if layer > 0:
            pair_stage(2 * layer)
        order = (xo, xa, xb, x)

        def in_weight_of(g):
            return weights[2 * layer, pl.ds(pl.multiple_of(g * GROUP_WIDTH, GROUP_WIDTH), GROUP_WIDTH)]

        for k, g in enumerate(order):
            product = lax.dot_general(
                cur[pl.ds(mates, taken)], in_weight_of(g), contract_cols,
                preferred_element_type=jnp.float32,
            )
            part[layer, k] = product.astype(jnp.bfloat16)
            send(part.at[layer, k], peer.at[layer, k], (part_send, part_recv), mate,
                 ((layer, k), (layer, k)))
        for k, g in enumerate(order):
            product = lax.dot_general(
                cur[pl.ds(mine, taken)], in_weight_of(g), contract_cols,
                preferred_element_type=jnp.float32,
            )
            arrive(peer.at[layer, k], (part_send, part_recv), ((layer, k), (layer, k)))
            total = (product + peer[layer, k].astype(jnp.float32)).astype(jnp.bfloat16)
            own[layer, k, 0] = total[:, :HALF]
            own[layer, k, 1] = total[:, HALF:]
            f = (first_send, first_recv)
            if k == 0:
                send(own.at[layer, 0, 0], first.at[layer, 0, 1], f, dev_a, ((layer, 0, 1), (layer, 0, 1)))
                send(own.at[layer, 0, 1], first.at[layer, 1, 1], f, dev_b, ((layer, 1, 1), (layer, 1, 1)))
            if k == 1:
                send(own.at[layer, 1, 0], first.at[layer, 0, 0], f, dev_a, ((layer, 0, 0), (layer, 0, 0)))
            if k == 2:
                send(own.at[layer, 2, 1], first.at[layer, 1, 0], f, dev_b, ((layer, 1, 0), (layer, 1, 0)))

        f = (first_send, first_recv)
        s = (second_send, second_recv)
        meanwhile(range(2 * LAYERS))
        for half, k, to in ((0, 2, dev_b), (1, 1, dev_a)):
            arrive(first.at[layer, half, 1], f, ((layer, half, 1), (layer, half, 1)))
            second_out[layer, half] = (
                own[layer, k, half].astype(jnp.float32) + first[layer, half, 1].astype(jnp.float32)
            ).astype(jnp.bfloat16)
            send(second_out.at[layer, half], second.at[layer, half], s, to, ((layer, half), (layer, half)))
        meanwhile(range(2 * LAYERS))
        pieces = []
        for half in range(2):
            arrive(first.at[layer, half, 0], f, ((layer, half, 0), (layer, half, 0)))
            arrive(second.at[layer, half], s, ((layer, half), (layer, half)))
            pieces.append(
                (
                    own[layer, 3, half].astype(jnp.float32)
                    + first[layer, half, 0].astype(jnp.float32)
                    + second[layer, half].astype(jnp.float32)
                ).astype(jnp.bfloat16)
            )
        hidden = jnp.concatenate(pieces, axis=1)
        pooled = lax.dot_general(band[...], hidden, contract, preferred_element_type=jnp.float32)
        pooled = (pooled * scale).astype(jnp.bfloat16)
        mixed = lax.dot_general(pooled, mix_ref[layer, x], contract, preferred_element_type=jnp.float32)
        gains = jnp.zeros((1, GROUP_WIDTH), jnp.float32)
        for g in range(GROUPS):
            of_g = gain_ref[pl.ds(layer, 1), pl.ds(g * GROUP_WIDTH, GROUP_WIDTH)]
            gains = jnp.where(x == g, of_g, gains)
        scaled = (mixed * gains).astype(jnp.bfloat16)
        gath[layer, core, x, 0] = scaled[:, :HALF]
        gath[layer, core, x, 1] = scaled[:, HALF:]

        def pass_on(g, half, to, slot):
            ref = gath.at[layer, core, g, half]
            send(ref, ref, (gath_send, gath_recv), to, ((layer, slot), (layer, core, g, half)))

        def take_in(side, g, half):
            arrive(gath.at[layer, side, g, half], (gath_send, gath_recv),
                   ((layer, 0), (layer, side, g, half)))

        pass_on(x, 0, dev_b, 0)
        pass_on(x, 1, dev_a, 1)
        pass_on(x, 0, dev_a, 2)
        pass_on(x, 1, dev_b, 3)
        pass_on(x, 0, mate, 4)
        pass_on(x, 1, mate, 5)
        meanwhile(range(2 * LAYERS))
        take_in(core, xb, 0)
        pass_on(xb, 0, dev_a, 6)
        take_in(core, xa, 1)
        pass_on(xa, 1, dev_b, 7)
        pass_on(xb, 0, mate, 8)
        pass_on(xa, 1, mate, 9)
        meanwhile(range(2 * LAYERS))
        take_in(core, xa, 0)
        pass_on(xa, 0, mate, 10)
        take_in(core, xb, 1)
        pass_on(xb, 1, mate, 11)
        take_in(core, xo, 0)
        pass_on(xo, 0, mate, 12)
        take_in(core, xo, 1)
        pass_on(xo, 1, mate, 13)

        def branch_of(side):
            whole = jnp.concatenate(
                [gath[layer, side, g, half] for g in range(GROUPS) for half in range(2)], axis=1
            )
            return lax.dot_general(
                whole, weights[2 * layer + 1], contract, preferred_element_type=jnp.float32
            )

        pair_stage(2 * layer + 1)
        summed[pl.ds(mine, given), :] = branch_of(core)
        for g in (x, xb, xa, xo):
            for half in range(2):
                take_in(1 - core, g, half)
        summed[pl.ds(mates, given), :] = branch_of(1 - core)

        stat_out[layer] = jnp.zeros((16, 128), jnp.float32)
        for b in range(7):
            here = pl.ds(b * rblock, rblock)
            value = summed[here, :] + alpha * cur[pl.ds(REACH + b * rblock, rblock), :].astype(jnp.float32)
            summed[here, :] = value
            for at_row, quantity in ((b, value), (8 + b, value * value)):
                total = jnp.sum(quantity, axis=1, keepdims=True)
                stat_out[layer, pl.ds(at_row, 1), :] = jnp.sum(
                    jnp.where(eye, total, 0.0), axis=0, keepdims=True
                )
        q = (stat_send, stat_recv)
        for step in range(1, n_tp):
            to = lax.rem(me + step, n_tp)
            send(stat_out.at[layer], stat_in.at[layer, me], q, to, ((layer, step), (layer, me)))
        stat_in[layer, me] = stat_out[layer]
        meanwhile(range(2 * LAYERS))
        for step in range(1, n_tp):
            other = lax.rem(me + step, n_tp)
            arrive(stat_in.at[layer, other], q, ((layer, step), (layer, other)))
        stats = stat_in[layer, 0]
        for k in range(1, n_tp):
            stats = stats + stat_in[layer, k]
        if layer == 0:
            halo.wait_send()
        mean = stats[0:8] / D
        var = stats[8:16] / D - mean * mean
        inverse = lax.rsqrt(var + epsilon)
        norm_gain = norm_gain_ref[pl.ds(layer, 1), :]
        norm_shift = norm_shift_ref[pl.ds(layer, 1), :]
        for b in range(7):
            mean_col = jnp.sum(jnp.where(eye, mean[b : b + 1], 0.0), axis=1, keepdims=True)
            inv_col = jnp.sum(jnp.where(eye, inverse[b : b + 1], 0.0), axis=1, keepdims=True)
            value = summed[pl.ds(b * rblock, rblock), :]
            value = (value - mean_col) * inv_col * norm_gain + norm_shift
            if layer < LAYERS - 1:
                cur[pl.ds(REACH + b * rblock, rblock), :] = value.astype(jnp.bfloat16)
            elif b == 0:
                out_ref[pl.ds(0, rblock - REACH), :] = value[REACH:].astype(jnp.bfloat16)
            else:
                out_ref[pl.ds(b * rblock - REACH, rblock), :] = value.astype(jnp.bfloat16)

    for copy in sent + sent_hops:
        copy.wait_send()


def per_device(n_sp, n_tp, stream, in_weight, out_weight, group_mix, pool_gain, norm_gain, norm_shift):
    rows, cols = stream.shape
    pool = GROUPS * GROUP_WIDTH
    share = (rows + REACH) // 2 - REACH // 2
    taken, given = share + HALO, share + REACH
    bf, f32 = jnp.bfloat16, jnp.float32
    classes = n_sp // STRIDE
    dma = pltpu.SemaphoreType.DMA
    return pl.pallas_call(
        functools.partial(kernel, n_sp, n_tp),
        out_shape=jax.ShapeDtypeStruct((rows, cols), bf),
        in_specs=[pl.BlockSpec(memory_space=pl.ANY)] * 7,
        out_specs=pl.BlockSpec(memory_space=pltpu.VMEM),
        scratch_shapes=[
            pltpu.VMEM(group_mix.shape, bf),
            pltpu.VMEM(pool_gain.shape, f32),
            pltpu.VMEM(norm_gain.shape, f32),
            pltpu.VMEM(norm_shift.shape, f32),
            pltpu.VMEM((2 * LAYERS, pool, cols), bf),
            pltpu.VMEM((rows + HALO, cols), bf),
            pltpu.VMEM((given, taken), bf),
            pltpu.VMEM((LAYERS, GROUPS, taken, GROUP_WIDTH), bf),
            pltpu.VMEM((LAYERS, GROUPS, taken, GROUP_WIDTH), bf),
            pltpu.VMEM((LAYERS, GROUPS, 2, taken, HALF), bf),
            pltpu.VMEM((LAYERS, 2, 2, taken, HALF), bf),
            pltpu.VMEM((LAYERS, 2, taken, HALF), bf),
            pltpu.VMEM((LAYERS, 2, taken, HALF), bf),
            pltpu.VMEM((LAYERS, 2, GROUPS, 2, given, HALF), bf),
            pltpu.VMEM((rows + REACH, cols), f32),
            pltpu.VMEM((LAYERS, 16, 128), f32),
            pltpu.VMEM((LAYERS, n_tp, 16, 128), f32),
            dma((9,)),
            dma((2 * LAYERS, 5, classes)),
            dma((2 * LAYERS, 5, classes)),
            dma((2 * LAYERS, 4, classes)),
            dma((2 * LAYERS, 4, classes)),
            dma((2,)),
            dma((LAYERS, GROUPS)),
            dma((LAYERS, GROUPS)),
            dma((LAYERS, 2, 2)),
            dma((LAYERS, 2, 2)),
            dma((LAYERS, 2)),
            dma((LAYERS, 2)),
            dma((LAYERS, 14)),
            dma((LAYERS, 2, GROUPS, 2)),
            dma((LAYERS, n_tp)),
            dma((LAYERS, n_tp)),
        ],
        compiler_params=pltpu.CompilerParams(
            collective_id=0, has_side_effects=True, vmem_limit_bytes=60 * 1024 * 1024
        ),
    )(stream, in_weight, out_weight, group_mix, pool_gain, norm_gain, norm_shift)


def solution(mesh):
    in_specs = (
        P(("grp", "sp"), "tp"),
        P(None, "sp", "tp"),
        P(None, "sp", "tp"),
        P(),
        P(),
        P(None, "tp"),
        P(None, "tp"),
    )
    out_specs = P(("grp", "sp"), "tp")
    return jax.shard_map(
        functools.partial(per_device, mesh.shape["sp"], mesh.shape["tp"]),
        mesh=mesh, in_specs=in_specs, out_specs=out_specs, check_vma=False,
    )
```

```python
import functools

import jax
import jax.numpy as jnp
from jax import lax
from jax.experimental import pallas as pl
from jax.experimental.pallas import tpu as pltpu
from jax.sharding import PartitionSpec as P

D = 4096
GROUPS = 4
GROUP_WIDTH = 256
LAYERS = 2
HALF = GROUP_WIDTH // 2
REACH = 16
STRIDE = 4
POLLS = (2, 4, 4, 4, 4, 40)
HALO = LAYERS * REACH
MESH = pl.DeviceIdType.MESH

epsilon = 1e-05


def kernel(
    n_sp,
    n_tp,
    stream_hbm,
    in_hbm,
    out_hbm,
    mix_hbm,
    gain_hbm,
    norm_gain_hbm,
    norm_shift_hbm,
    out_ref,
    mix_ref,
    gain_ref,
    norm_gain_ref,
    norm_shift_ref,
    weights,
    cur,
    band,
    part,
    peer,
    own,
    first,
    second_out,
    second,
    gath,
    summed,
    stat_out,
    stat_in,
    load_sem,
    ring_send,
    ring_recv,
    many_recv,
    pair_send,
    pair_recv,
    halo_sem,
    part_send,
    part_recv,
    first_send,
    first_recv,
    second_send,
    second_recv,
    gath_send,
    gath_recv,
    stat_send,
    stat_recv,
):
    rows = stream_hbm.shape[0]
    block = in_hbm.shape[1]
    share = (rows + REACH) // 2 - REACH // 2
    taken = share + HALO
    given = share + REACH
    z = lax.axis_index("sp")
    me = lax.axis_index("tp")
    part_at = lax.axis_index("grp")
    core = lax.rem(me, 2)
    x = me // 2
    mate = me + 1 - 2 * core
    xa = x + 1 - 2 * lax.rem(x, 2)
    xb = GROUPS - 1 - x
    xo = lax.rem(x + 2, GROUPS)
    dev_a = 2 * xa + core
    dev_b = 2 * xb + core
    alpha = (2.0 * LAYERS) ** 0.25

    def load(src, dst, index):
        copy = pltpu.make_async_copy(src, dst, load_sem.at[index])
        copy.start()
        return copy

    own_rows = pl.ds(pl.multiple_of(z * block, block), block)
    loads = [
        load(in_hbm.at[0], weights.at[0, own_rows], 0),
        load(out_hbm.at[0], weights.at[1, own_rows], 1),
        load(in_hbm.at[1], weights.at[2, own_rows], 2),
        load(out_hbm.at[1], weights.at[3, own_rows], 3),
        load(stream_hbm, cur.at[pl.ds(HALO, rows)], 4),
        load(mix_hbm, mix_ref, 5),
        load(gain_hbm, gain_ref, 6),
        load(norm_gain_hbm, norm_gain_ref, 7),
        load(norm_shift_hbm, norm_shift_ref, 8),
    ]

    barrier = pltpu.get_barrier_semaphore()
    reached = (1, -1, STRIDE, -STRIDE)
    for distance in reached:
        pl.semaphore_signal(
            barrier, inc=1, device_id={"sp": lax.rem(z + distance % n_sp, n_sp)}, device_id_type=MESH
        )
    for step in range(1, n_tp):
        pl.semaphore_signal(
            barrier, inc=1, device_id={"tp": lax.rem(me + step, n_tp)}, device_id_type=MESH
        )
    beside = part_at + 1 - 2 * lax.rem(part_at, 2)
    pl.semaphore_signal(barrier, inc=1, device_id={"grp": beside}, device_id_type=MESH)
    pl.semaphore_wait(barrier, len(reached) + 1 + n_tp - 1)

    classes = n_sp // STRIDE
    main_steps, back_steps = classes // 2, (classes - 1) // 2

    def at(array, owner):
        return weights.at[array, pl.ds(pl.multiple_of(owner * block, block), block)]

    def along(distance):
        return lax.rem(z + distance % n_sp, n_sp)

    half_block = block // 2
    carried = lax.rem(part_at, 2)
    beside = part_at + 1 - 2 * carried

    def half_at(array, owner, which):
        start = owner * block + which * half_block
        return weights.at[array, pl.ds(pl.multiple_of(start, half_block), half_block)]

    def across(array, kind, index, owner, which):
        ref = half_at(array, owner, which)
        return pltpu.make_async_remote_copy(
            src_ref=ref,
            dst_ref=ref,
            send_sem=pair_send.at[array],
            recv_sem=pair_recv.at[array],
            device_id={"grp": beside},
            device_id_type=MESH,
        )

    def hop(array, kind, index, owner, to):
        ref = half_at(array, owner, carried)
        return pltpu.make_async_remote_copy(
            src_ref=ref,
            dst_ref=ref,
            send_sem=ring_send.at[array],
            recv_sem=(
                many_recv.at[array, kind - 3]
                if kind > 2
                else ring_recv.at[array, (0, main_steps, main_steps + back_steps)[kind] + index]
            ),
            device_id={"sp": to},
            device_id_type=MESH,
        )

    def go(array, kind, index, owner, distance):
        hop(array, kind, index, owner, along(distance)).start()

    pair_kind = (0, 0, 1, 2, 3)

    def come(array, kind, index, owner):
        hop(array, kind, index, owner, along(1)).wait_recv()

    held_back = [[] for _ in range(2 * LAYERS)]

    def share_out(array, kind, index, owner):
        copy = across(array, pair_kind[kind], index, owner, carried)
        if array == 0:
            copy.start()
        else:
            held_back[array].append(copy)

    def let_go(arrays):
        for array in arrays:
            for copy in held_back[array]:
                copy.start()
            held_back[array].clear()

    def both(k):
        found = [(k, -STRIDE * k)] if k <= main_steps else []
        if 0 < k <= back_steps:
            found.append((classes - k, STRIDE * k))
        return found

    def stride_stage(array, k):
        for index, distance in both(k):
            kind = 0 if distance <= 0 else 1
            owner = along(distance)
            if k > 0:
                come(array, kind, k - 1, owner)
            if (kind == 0) and k < main_steps:
                go(array, 0, k, owner, STRIDE)
            if (kind == 1 or k == 0) and k < back_steps:
                go(array, 1, k, owner, -STRIDE)
            go(array, 2, index, owner, -1)
            go(array, 4, index, owner, 1)
            if k > 0:
                share_out(array, kind, index, owner)

    def near_stage(array, k):
        for index, distance in both(k):
            owner = along(distance + 1)
            come(array, 2, index, owner)
            go(array, 3, index, owner, -1)
            share_out(array, 2, index, owner)

    def wait_many(array, pieces, send_sem, recv_sem):
        ref = weights.at[array, pl.ds(0, pieces * half_block)]
        return pltpu.make_async_remote_copy(
            src_ref=ref,
            dst_ref=ref,
            send_sem=send_sem,
            recv_sem=recv_sem,
            device_id={"grp": beside},
            device_id_type=MESH,
        )

    def last_stage(array, kind, shift):
        wait_many(array, classes, ring_send.at[array], many_recv.at[array, kind - 3]).wait_recv()
        for k in range(main_steps + 1):
            for index, distance in both(k):
                share_out(array, kind, index, along(distance + shift))

    def pair_stage(array):
        wait_many(array, n_sp - 1, pair_send.at[array], pair_recv.at[array]).wait_recv()

    def stages(array):
        found = []
        for k in range(1, main_steps + 1):
            found.append(functools.partial(stride_stage, array, k))
            if k > 1:
                found.append(functools.partial(near_stage, array, k - 2))
        for k in range(max(main_steps - 1, 0), main_steps + 1):
            found.append(functools.partial(near_stage, array, k))
        found.append(functools.partial(last_stage, array, 4, -1))
        found.append(functools.partial(last_stage, array, 3, 2))
        return found

    for array in range(2):
        loads[array].wait()
        stride_stage(array, 0)
    loads[4].wait()
    halo = pltpu.make_async_remote_copy(
        src_ref=cur.at[pl.ds(rows, HALO)],
        dst_ref=cur.at[pl.ds(0, HALO)],
        send_sem=halo_sem.at[0],
        recv_sem=halo_sem.at[1],
        device_id={"sp": lax.rem(z + 1, n_sp)},
        device_id_type=MESH,
    )
    halo.start()
    for array in range(2, 4):
        loads[array].wait()

    window = 2 * jnp.where(x == 0, 1, jnp.where(x == 1, 2, jnp.where(x == 2, 4, 8)))
    start = z * rows - HALO + core * share
    r = lax.broadcasted_iota(jnp.int32, (given, taken), 0) + REACH
    j = lax.broadcasted_iota(jnp.int32, (given, taken), 1)
    count = jnp.clip(start + r + 1, 1, window)
    inside = (r - j >= 0) & (r - j < window) & (start + j >= 0)
    entry = jnp.where(inside, 1.0, 0.0) - jnp.where(r == j, count.astype(jnp.float32), 0.0)
    band[...] = entry.astype(jnp.bfloat16)
    column = lax.broadcasted_iota(jnp.int32, (given, 1), 0) + REACH + start + 1
    scale = 1.0 / jnp.clip(column, 1, window).astype(jnp.float32)

    waves = [stages(array) for array in range(2 * LAYERS)]
    turns = sorted(
        (k if array < 2 else 8 if k == 0 else len(waves[0]) + k, array, k)
        for array in range(2 * LAYERS)
        for k in range(len(waves[array]))
    )
    done = len(waves[0])
    for turn, array, k in turns:
        if turn == 4 and array == 0:
            stride_stage(2, 0)
            stride_stage(3, 0)
        if turn < done:
            waves[array][k]()
    later = [waves[array][k] for turn, array, k in turns if turn >= done]
    polls = list(POLLS)

    def meanwhile(arrays):
        for _ in range(polls.pop(0) if polls else len(later)):
            if later:
                later.pop(0)()
        let_go(arrays)

    for load in loads[5:]:
        load.wait()
    pair_stage(0)
    halo.wait_recv()
    meanwhile((1,))

    def send(src, dst, sems, to, layer, index):
        pltpu.make_async_remote_copy(
            src_ref=src,
            dst_ref=dst,
            send_sem=sems[0].at[layer],
            recv_sem=sems[1].at[index],
            device_id={"tp": to},
            device_id_type=MESH,
        ).start()

    def waiting(ref, sems, layer, index):
        return pltpu.make_async_remote_copy(
            src_ref=ref,
            dst_ref=ref,
            send_sem=sems[0].at[layer],
            recv_sem=sems[1].at[index],
            device_id={"tp": mate},
            device_id_type=MESH,
        )

    def arrive(ref, sems, layer, index):
        waiting(ref, sems, layer, index).wait_recv()

    contract_cols = (((1,), (1,)), ((), ()))
    contract = (((1,), (0,)), ((), ()))
    mine = pl.multiple_of(core * share, REACH)
    mates = pl.multiple_of((1 - core) * share, REACH)
    rblock = (rows + REACH) // 7
    eye = lax.broadcasted_iota(jnp.int32, (rblock, 128), 0) == lax.broadcasted_iota(
        jnp.int32, (rblock, 128), 1
    )

    def piece(side, g, half):
        return (side * GROUPS + g) * 2 + half

    for layer in range(LAYERS):
        if layer > 0:
            pair_stage(2 * layer)
        order = (xo, xa, xb, x)

        def in_weight_of(g):
            return weights[2 * layer, pl.ds(pl.multiple_of(g * GROUP_WIDTH, GROUP_WIDTH), GROUP_WIDTH)]

        p = (part_send, part_recv)
        f = (first_send, first_recv)
        s = (second_send, second_recv)
        c = (gath_send, gath_recv)
        q = (stat_send, stat_recv)

        def product_of(k):
            of_g = in_weight_of(order[k])
            product = lax.dot_general(cur[...], of_g, contract_cols, preferred_element_type=jnp.float32)
            part[layer, k] = product.astype(jnp.bfloat16)
            send(part.at[layer, k, pl.ds(mates, taken)], peer.at[layer, k], p, mate, layer, (layer, k))

        def reduce_pair(k):
            arrive(peer.at[layer, k], p, layer, (layer, k))
            total = (
                part[layer, k, pl.ds(mine, taken)].astype(jnp.float32) + peer[layer, k].astype(jnp.float32)
            ).astype(jnp.bfloat16)
            own[layer, k, 0] = total[:, :HALF]
            own[layer, k, 1] = total[:, HALF:]
            if k == 0:
                send(own.at[layer, 0, 0], first.at[layer, 0, 1], f, dev_a, layer, (layer, 0, 1))
                send(own.at[layer, 0, 1], first.at[layer, 1, 1], f, dev_b, layer, (layer, 1, 1))
            if k == 1:
                send(own.at[layer, 1, 0], first.at[layer, 0, 0], f, dev_a, layer, (layer, 0, 0))
            if k == 2:
                send(own.at[layer, 2, 1], first.at[layer, 1, 0], f, dev_b, layer, (layer, 1, 0))

        product_of(0)
        product_of(1)
        product_of(2)
        reduce_pair(0)
        product_of(3)
        reduce_pair(1)
        reduce_pair(2)
        reduce_pair(3)
        meanwhile(range(2 * LAYERS))
        for half, k, to in ((0, 2, dev_b), (1, 1, dev_a)):
            arrive(first.at[layer, half, 1], f, layer, (layer, half, 1))
            second_out[layer, half] = (
                own[layer, k, half].astype(jnp.float32) + first[layer, half, 1].astype(jnp.float32)
            ).astype(jnp.bfloat16)
            send(second_out.at[layer, half], second.at[layer, half], s, to, layer, (layer, half))
        meanwhile(range(2 * LAYERS))
        pieces = []
        for half in range(2):
            arrive(first.at[layer, half, 0], f, layer, (layer, half, 0))
            arrive(second.at[layer, half], s, layer, (layer, half))
            pieces.append(
                (
                    own[layer, 3, half].astype(jnp.float32)
                    + first[layer, half, 0].astype(jnp.float32)
                    + second[layer, half].astype(jnp.float32)
                ).astype(jnp.bfloat16)
            )
        hidden = jnp.concatenate(pieces, axis=1)
        pooled = lax.dot_general(band[...], hidden, contract, preferred_element_type=jnp.float32)
        pooled = (pooled * scale).astype(jnp.bfloat16)
        mixed = lax.dot_general(pooled, mix_ref[layer, x], contract, preferred_element_type=jnp.float32)
        gains = jnp.zeros((1, GROUP_WIDTH), jnp.float32)
        for g in range(GROUPS):
            of_g = gain_ref[pl.ds(layer, 1), pl.ds(g * GROUP_WIDTH, GROUP_WIDTH)]
            gains = jnp.where(x == g, of_g, gains)
        scaled = (mixed * gains).astype(jnp.bfloat16)
        gath[layer, piece(core, x, 0)] = scaled[:, :HALF]
        gath[layer, piece(core, x, 1)] = scaled[:, HALF:]

        def pass_on(g, half, to):
            ref = gath.at[layer, piece(core, g, half)]
            index = 2 * GROUPS if to is mate else 2 * g + half
            send(ref, ref, c, to, layer, (layer, index))

        def take_in(g, half):
            arrive(gath.at[layer, piece(core, g, half)], c, layer, (layer, 2 * g + half))

        pass_on(x, 0, dev_b)
        pass_on(x, 1, dev_a)
        pass_on(x, 0, dev_a)
        pass_on(x, 1, dev_b)
        pass_on(x, 0, mate)
        pass_on(x, 1, mate)
        meanwhile(range(2 * LAYERS))
        take_in(xb, 0)
        pass_on(xb, 0, dev_a)
        take_in(xa, 1)
        pass_on(xa, 1, dev_b)
        pass_on(xb, 0, mate)
        pass_on(xa, 1, mate)
        meanwhile(range(2 * LAYERS))
        take_in(xa, 0)
        pass_on(xa, 0, mate)
        take_in(xb, 1)
        pass_on(xb, 1, mate)
        take_in(xo, 0)
        pass_on(xo, 0, mate)
        take_in(xo, 1)
        pass_on(xo, 1, mate)

        def branch_of(side):
            whole = jnp.concatenate(
                [gath[layer, piece(side, g, half)] for g in range(GROUPS) for half in range(2)], axis=1
            )
            return lax.dot_general(
                whole, weights[2 * layer + 1], contract, preferred_element_type=jnp.float32
            )

        pair_stage(2 * layer + 1)
        summed[pl.ds(mine, given), :] = branch_of(core)
        arrive(gath.at[layer, pl.ds(piece(1 - core, 0, 0), 2 * GROUPS)], c, layer, (layer, 2 * GROUPS))
        summed[pl.ds(mates, given), :] = branch_of(1 - core)

        stat_out[layer] = jnp.zeros((16, 128), jnp.float32)
        for b in range(7):
            here = pl.ds(b * rblock, rblock)
            value = summed[here, :] + alpha * cur[pl.ds(REACH + b * rblock, rblock), :].astype(jnp.float32)
            summed[here, :] = value
            for at_row, quantity in ((b, value), (8 + b, value * value)):
                total = jnp.sum(quantity, axis=1, keepdims=True)
                stat_out[layer, pl.ds(at_row, 1), :] = jnp.sum(
                    jnp.where(eye, total, 0.0), axis=0, keepdims=True
                )
        for step in range(1, n_tp):
            to = lax.rem(me + step, n_tp)
            send(stat_out.at[layer], stat_in.at[layer, me], q, to, layer, layer)
        stat_in[layer, me] = stat_out[layer]
        meanwhile(range(2 * LAYERS))
        arrive(stat_in.at[layer, pl.ds(0, n_tp - 1)], q, layer, layer)
        stats = stat_in[layer, 0]
        for k in range(1, n_tp):
            stats = stats + stat_in[layer, k]
        if layer == 0:
            halo.wait_send()
        mean = stats[0:8] / D
        var = stats[8:16] / D - mean * mean
        inverse = lax.rsqrt(var + epsilon)
        norm_gain = norm_gain_ref[pl.ds(layer, 1), :]
        norm_shift = norm_shift_ref[pl.ds(layer, 1), :]
        for b in range(7):
            mean_col = jnp.sum(jnp.where(eye, mean[b : b + 1], 0.0), axis=1, keepdims=True)
            inv_col = jnp.sum(jnp.where(eye, inverse[b : b + 1], 0.0), axis=1, keepdims=True)
            value = summed[pl.ds(b * rblock, rblock), :]
            value = (value - mean_col) * inv_col * norm_gain + norm_shift
            if layer < LAYERS - 1:
                cur[pl.ds(REACH + b * rblock, rblock), :] = value.astype(jnp.bfloat16)
            elif b == 0:
                out_ref[pl.ds(0, rblock - REACH), :] = value[REACH:].astype(jnp.bfloat16)
            else:
                out_ref[pl.ds(b * rblock - REACH, rblock), :] = value.astype(jnp.bfloat16)

    for layer in range(LAYERS):
        waiting(peer.at[layer], p, layer, (layer, 0)).wait_send()
        waiting(first.at[layer], f, layer, (layer, 0, 0)).wait_send()
        waiting(second.at[layer], s, layer, (layer, 0)).wait_send()
        waiting(gath.at[layer, pl.ds(0, 4 * GROUPS - 2)], c, layer, (layer, 0)).wait_send()
        waiting(stat_in.at[layer, pl.ds(0, n_tp - 1)], q, layer, layer).wait_send()
    for array in range(2 * LAYERS):
        wait_many(array, n_sp - 1, ring_send.at[array], pair_recv.at[array]).wait_send()
        wait_many(array, n_sp - 1, pair_send.at[array], pair_recv.at[array]).wait_send()


def per_device(n_sp, n_tp, stream, in_weight, out_weight, group_mix, pool_gain, norm_gain, norm_shift):
    rows, cols = stream.shape
    pool = GROUPS * GROUP_WIDTH
    share = (rows + REACH) // 2 - REACH // 2
    taken, given = share + HALO, share + REACH
    bf, f32 = jnp.bfloat16, jnp.float32
    classes = n_sp // STRIDE
    dma = pltpu.SemaphoreType.DMA
    return pl.pallas_call(
        functools.partial(kernel, n_sp, n_tp),
        out_shape=jax.ShapeDtypeStruct((rows, cols), bf),
        in_specs=[pl.BlockSpec(memory_space=pl.ANY)] * 7,
        out_specs=pl.BlockSpec(memory_space=pltpu.VMEM),
        scratch_shapes=[
            pltpu.VMEM(group_mix.shape, bf),
            pltpu.VMEM(pool_gain.shape, f32),
            pltpu.VMEM(norm_gain.shape, f32),
            pltpu.VMEM(norm_shift.shape, f32),
            pltpu.VMEM((2 * LAYERS, pool, cols), bf),
            pltpu.VMEM((rows + HALO, cols), bf),
            pltpu.VMEM((given, taken), bf),
            pltpu.VMEM((LAYERS, GROUPS, rows + HALO, GROUP_WIDTH), bf),
            pltpu.VMEM((LAYERS, GROUPS, taken, GROUP_WIDTH), bf),
            pltpu.VMEM((LAYERS, GROUPS, 2, taken, HALF), bf),
            pltpu.VMEM((LAYERS, 2, 2, taken, HALF), bf),
            pltpu.VMEM((LAYERS, 2, taken, HALF), bf),
            pltpu.VMEM((LAYERS, 2, taken, HALF), bf),
            pltpu.VMEM((LAYERS, 4 * GROUPS, given, HALF), bf),
            pltpu.VMEM((rows + REACH, cols), f32),
            pltpu.VMEM((LAYERS, 16, 128), f32),
            pltpu.VMEM((LAYERS, n_tp, 16, 128), f32),
            dma((9,)),
            dma((2 * LAYERS,)),
            dma((2 * LAYERS, 2 * classes)),
            dma((2 * LAYERS, 2)),
            dma((2 * LAYERS,)),
            dma((2 * LAYERS,)),
            dma((2,)),
            dma((LAYERS,)),
            dma((LAYERS, GROUPS)),
            dma((LAYERS,)),
            dma((LAYERS, 2, 2)),
            dma((LAYERS,)),
            dma((LAYERS, 2)),
            dma((LAYERS,)),
            dma((LAYERS, 2 * GROUPS + 1)),
            dma((LAYERS,)),
            dma((LAYERS,)),
        ],
        compiler_params=pltpu.CompilerParams(
            collective_id=0, has_side_effects=True, vmem_limit_bytes=60 * 1024 * 1024
        ),
    )(stream, in_weight, out_weight, group_mix, pool_gain, norm_gain, norm_shift)


def solution(mesh):
    in_specs = (
        P(("grp", "sp"), "tp"),
        P(None, "sp", "tp"),
        P(None, "sp", "tp"),
        P(),
        P(),
        P(None, "tp"),
        P(None, "tp"),
    )
    out_specs = P(("grp", "sp"), "tp")
    return jax.shard_map(
        functools.partial(per_device, mesh.shape["sp"], mesh.shape["tp"]),
        mesh=mesh, in_specs=in_specs, out_specs=out_specs, check_vma=False,
    )
```
